512 devices in a mesh: fs: 64 (over z, y), tp: 8 (over x, core).
Axes of the slice: x: 4, y: 4, z: 16, core: 2. Of those that a mesh axis runs over, the one named last changes fastest.
Arguments:
- inputs: bfloat16 [16384, 2048], P('fs'), may hold values from -6 to 6
- query_cot: bfloat16 [16384, 1024], P('fs', 'tp'), may hold values from -0.046875 to 0.046875
- query_basis: bfloat16 [2048, 256], P('fs'), may hold values from -0.125 to 0.125
- query_master: float32 [2048, 1024], P('fs', 'tp'), may hold values from -3 to 3
- query_first: float32 [256, 1024], P('fs', 'tp'), may hold values from -4 to 4
- query_second: float32 [256, 1024], P('fs', 'tp'), may hold values from 0.02 to 4
Outputs:
- query_step: float32 [2048, 1024], P('fs', 'tp')
- query_first_new: float32 [256, 1024], P('fs', 'tp')
- query_second_new: float32 [256, 1024], P('fs', 'tp')
- query_copy: bfloat16 [2048, 1024], P('fs', 'tp')
The draws below stay inside these ranges and needn't reach their ends.
All inputs are finite; a program needn't handle non-finite values.
Results may differ from the reference program's by a relative error of at most 0.0011.
Values may be sent and summed in bfloat16 or wider, within the bound.
A program may use at most 64 MiB of HBM per device.

```python
import math
import jax
import jax.numpy as jnp
from jax import lax

D = 2048
HEADS = 8
DQK = 128
RANK = 256
TOK_DEV = 256
TOKENS = 16384
NQ = 1024
N_FS = 64


def levels(key, extent, pieces, least, top_value):
    def one(position, blocks):
        heights = jax.random.uniform(jax.random.fold_in(jax.random.fold_in(key, 6), position), (blocks,), jnp.float32, least / len(pieces), top_value / len(pieces))
        return jnp.repeat(jnp.exp(heights), extent[position] // blocks).reshape((-1,) + (1,) * (len(extent) - position - 1))

    level = one(*pieces[0])
    for cut in pieces[1:]:
        level = level * one(*cut)
    return level


def scatter_about(rng, dims, spread, reach, pieces=(), dtype=jnp.bfloat16):
    values = jax.random.normal(rng, dims, jnp.float32) * spread
    if len(pieces) > 0:
        values = levels(rng, dims, pieces, -0.22, 0.18) * values
    return jnp.clip(values, min=-reach, max=reach).astype(dtype)


def setup_inputs(seed: int = 0) -> dict:
    streams_of = jax.random.split(jax.random.key(seed), 7)
    return {
        "inputs": scatter_about(streams_of[0], (TOKENS, D), 1.0, 6.0, ((0, 64),)),
        "query_cot": scatter_about(streams_of[1], (TOKENS, NQ), (1.0 / (TOK_DEV * N_FS) ** 0.5), 0.046875, ((0, 64), (1, 8))),
        "query_basis": scatter_about(streams_of[2], (D, RANK), D ** -0.5, 0.125, ((0, 64),)),
        "query_master": scatter_about(streams_of[3], (D, NQ), 0.5, 3.0, ((0, 64), (1, 8)), jnp.float32),
        "query_first": scatter_about(streams_of[4], (RANK, NQ), 1.0, 4.0, ((0, 64), (1, 8)), jnp.float32),
        "query_second": jnp.clip(jnp.exp(math.log(4.0) - 5.2983174 * jax.random.uniform(streams_of[5], (RANK, NQ), jnp.float32) ** levels(streams_of[5], (RANK, NQ), ((0, 64), (1, 8)), -0.2, 0.2)), 0.02, 4.0),
    }


def moments(first, second, low_grad):
    first_new = 0.8 * first + 0.2 * low_grad
    second_new = 0.9 * second + 0.1 * low_grad * low_grad
    return (first_new, second_new, first_new / jnp.sqrt(second_new))

def scaled(update, width):
    shaped = update.reshape(RANK, HEADS, width)
    head_mean = lax.optimization_barrier(jnp.mean(shaped * shaped, axis=(0, 2)))
    whole_mean = jnp.mean(update * update)
    factor = 1.0 / jnp.sqrt(head_mean + whole_mean)
    return (shaped * factor[None, :, None]).reshape(RANK, HEADS * width)

def reference(inputs, query_cot, query_basis, query_master, query_first, query_second):
    gradient = jnp.dot(inputs.T, query_cot, preferred_element_type=jnp.float32)
    basis_wide = query_basis.astype(jnp.float32)
    low_grad = jnp.dot(basis_wide.T, gradient, precision=lax.Precision.HIGHEST)
    first_new, second_new, update = moments(query_first, query_second, low_grad)
    step_full = jnp.dot(basis_wide, scaled(update, DQK), precision=lax.Precision.HIGHEST)
    copy_new = (query_master + step_full).astype(jnp.bfloat16)
    return (step_full, first_new, second_new, copy_new)
```

```python
import functools

import jax
import jax.numpy as jnp
from jax import lax
from jax.experimental import pallas as pl
from jax.experimental.pallas import tpu as pltpu
from jax.sharding import PartitionSpec as P

DQK = 128
NY = 4
REACH = 4
LANES = 128
MESH = pl.DeviceIdType.MESH


def split2(value):
    high = value.astype(jnp.bfloat16)
    low = (value - high.astype(jnp.float32)).astype(jnp.bfloat16)
    return high, low


def moments(first, second, low):
    return 0.8 * first + 0.2 * low, 0.9 * second + 0.1 * low * low


def kernel(
    nz, ny, tp,
    inputs_ref, cot_ref, basis_ref, first_ref, second_ref,
    product_ref, factor_ref, low_ref,
    xv, cv, bv, fv, sv, gbuf, mbuf, part, rbuf, zsend, zbuf, ubuf, ufull, sums,
    load_sem, z_send, z_recv, w_send, w_recv, y_send, y_recv, c_send, c_recv,
    r_send, r_recv, s_send, s_recv, u_send, u_recv, v_send, v_recv, q_send, q_recv,
):
    me = lax.axis_index("fs")
    t = lax.axis_index("tp")
    z, y = me // ny, me % ny
    rr, cols = first_ref.shape
    rows, rank = basis_ref.shape
    tokens = inputs_ref.shape[0]
    group = rank // tp
    packs = LANES // group
    low_z = nz // 2 - 1
    f32, bf16 = jnp.float32, jnp.bfloat16

    def fs_at(dz, dy):
        return (z + dz) % nz * ny + (y + dy) % ny

    def remote(src, dst, send, recv, fs, core):
        return pltpu.make_async_remote_copy(
            src_ref=src, dst_ref=dst, send_sem=send, recv_sem=recv,
            device_id=(fs, core), device_id_type=MESH,
        )

    loads = [
        pltpu.make_async_copy(basis_ref, bv, load_sem.at[0]),
        pltpu.make_async_copy(cot_ref, cv.at[t], load_sem.at[1]),
        pltpu.make_async_copy(inputs_ref, xv, load_sem.at[2]),
        pltpu.make_async_copy(first_ref, fv, load_sem.at[3]),
        pltpu.make_async_copy(second_ref, sv, load_sem.at[4]),
    ]
    for load in loads:
        load.start()

    near = [d for k in range(REACH, 0, -1) for d in (k, -k)]
    barrier = pltpu.get_barrier_semaphore()
    for d in near:
        pl.semaphore_signal(barrier, inc=1, device_id=(fs_at(d, 0), t), device_id_type=MESH)
    for d in range(1, ny):
        pl.semaphore_signal(barrier, inc=1, device_id=(fs_at(0, d), t), device_id_type=MESH)
    for d in range(1, tp):
        pl.semaphore_signal(barrier, inc=1, device_id=(me, (t + d) % tp), device_id_type=MESH)

    loads[0].wait()
    half = t // packs
    spot = t % packs
    wide = jnp.where(half == 0, bv[:, :LANES].astype(f32), bv[:, LANES:].astype(f32))
    lane = lax.broadcasted_iota(jnp.int32, (8, LANES), 1) // group
    packed = jnp.zeros((8, LANES), f32)
    for k in range(packs):
        moved = pltpu.roll(wide[8 * k : 8 * k + 8], (LANES + group * k - group * spot) % LANES, 1)
        packed = jnp.where(lane == k, moved, packed)
    gbuf[y, low_z] = packed.astype(bf16)

    pl.semaphore_wait(barrier, len(near) + ny - 1 + tp - 1)

    sent = []

    def go(copy):
        copy.start()
        sent.append(copy)

    own = gbuf.at[y, low_z]
    for i, d in enumerate(near):
        go(remote(own, gbuf.at[y, low_z - d], z_send.at[i], z_recv.at[low_z - d], fs_at(d, 0), t))
    loads[1].wait()
    for d in range(1, tp):
        to = (t + d) % tp
        go(remote(cv.at[t], cv.at[t], c_send.at[d], c_recv.at[t], me, to))

    def arrived(d):
        remote(own, gbuf.at[y, low_z + d], z_send.at[0], z_recv.at[low_z + d], me, t).wait_recv()

    for d in range(1, REACH + 1):
        arrived(d)
    go(remote(
        gbuf.at[y, pl.ds(low_z + 1, REACH)], gbuf.at[y, pl.ds(low_z + 1 + REACH, REACH)],
        w_send.at[0], w_recv.at[0], fs_at(-REACH, 0), t,
    ))
    for d in range(1, REACH):
        arrived(-d)
    go(remote(
        gbuf.at[y, pl.ds(low_z + 1 - REACH, REACH - 1)], gbuf.at[y, pl.ds(low_z + 1 - 2 * REACH, REACH - 1)],
        w_send.at[1], w_recv.at[1], fs_at(REACH, 0), t,
    ))
    arrived(-REACH)

    spans = [
        (low_z - REACH, 2 * REACH + 1),
        (low_z + 1 + REACH, REACH),
        (0, REACH - 1),
    ]

    def spread(s):
        span = pl.ds(*spans[s])
        for d in range(1, ny):
            go(remote(
                gbuf.at[y, span], gbuf.at[y, span], y_send.at[s, d], y_recv.at[s, y], fs_at(0, d), t
            ))

    def gathered(s):
        span = pl.ds(*spans[s])
        for d in range(1, ny):
            k = (y + d) % ny
            remote(gbuf.at[k, span], gbuf.at[k, span], y_send.at[s, 0], y_recv.at[s, k], me, t).wait_recv()

    def unpack(s):
        start, count = spans[s]
        for slot in range(start, start + count):
            for k in range(ny):
                block = gbuf[k, slot].astype(f32)
                rows_of = [jnp.where(lane == i, block, 0.0) for i in range(packs)]
                at = pl.multiple_of((z + slot - low_z + nz) % nz * (ny * rows) + k * rows, rows)
                mbuf[pl.ds(at, rows), :] = jnp.concatenate(rows_of, axis=0).astype(bf16)

    spread(0)
    far = pl.ds(low_z + 1 + REACH, REACH)
    remote(gbuf.at[y, far], gbuf.at[y, far], w_send.at[0], w_recv.at[0], me, t).wait_recv()
    spread(1)
    far = pl.ds(0, REACH - 1)
    remote(gbuf.at[y, far], gbuf.at[y, far], w_send.at[1], w_recv.at[1], me, t).wait_recv()
    spread(2)
    gathered(0)
    unpack(0)
    loads[2].wait()
    for s in (1, 2):
        gathered(s)
        unpack(s)

    wide = jnp.dot(xv[...], mbuf[...], preferred_element_type=f32)
    shift = LANES // 2
    while shift >= group:
        wide += pltpu.roll(wide, shift, 1)
        shift //= 2
    turned = jnp.transpose(wide)[:group]
    per_y = group // ny // rr
    turned = jnp.concatenate(
        [turned[(j * ny + k) * rr : (j * ny + k + 1) * rr] for k in range(ny) for j in range(per_y)], axis=0
    )
    stacked = jnp.concatenate(split2(turned), axis=0)

    tall = per_y * rr
    for d in list(range(1, tp)) + [0]:
        to = (t + d) % tp
        if d > 0:
            remote(cv.at[to], cv.at[to], c_send.at[0], c_recv.at[to], me, t).wait_recv()
        share = jnp.dot(stacked, cv[to], preferred_element_type=f32)
        share = share[:group] + share[group:]
        for k in range(ny):
            part[k, to] = share[k * tall : (k + 1) * tall]
        for e in list(range(1, ny)) + [0]:
            k = (y + e) % ny
            if d > 0 or e > 0:
                go(remote(
                    part.at[k, to], rbuf.at[y, t], r_send.at[d, e], r_recv.at[y, t], fs_at(0, e), to
                ))

    rbuf[y, t] = part[y, t]
    for i in range(tp):
        total = None
        for k in range(ny):
            @pl.when(jnp.logical_or(k != y, i != t))
            def _():
                remote(part.at[k, i], rbuf.at[k, i], r_send.at[0, 0], r_recv.at[k, i], me, t).wait_recv()

            total = rbuf[k, i] if total is None else total + rbuf[k, i]
        for j in range(per_y):
            zz = i * per_y + j
            zsend[zz] = total[j * rr : (j + 1) * rr]

            @pl.when(zz != z)
            def _():
                remote(zsend.at[zz], zbuf.at[z], s_send.at[zz], s_recv.at[z], zz * ny + y, t).start()

    for load in loads[3:]:
        load.wait()
    for copy in sent:
        copy.wait_send()
    sent.clear()

    low = zsend[z]
    for d in range(1, nz):
        zz = (z + d) % nz
        remote(zsend.at[z], zbuf.at[zz], s_send.at[zz], s_recv.at[zz], me, t).wait_recv()
        low += zbuf[zz]

    first_new, second_new = moments(fv[...], sv[...], low)
    update = first_new / jnp.sqrt(second_new)
    ubuf[y, low_z] = update
    own = ubuf.at[y, low_z]
    order = [nz // 2] + [d for k in range(nz // 2 - 1, 0, -1) for d in (k, -k)]
    for i, d in enumerate(order):
        slot = low_z - d + (nz if low_z - d < 0 else 0)
        go(remote(own, ubuf.at[y, slot], u_send.at[i], u_recv.at[slot], fs_at(d, 0), t))
    low_ref[...] = low
    for d in range(1, nz):
        zz = (z + d) % nz
        remote(zsend.at[zz], zbuf.at[z], s_send.at[zz], s_recv.at[z], zz * ny + y, t).wait_send()

    groups = [(low_z - 3, 7), (low_z + 4, 3), (low_z - 5, 2), (low_z + 7, 2), (0, 2)]
    squares = update * update
    for g, (start, count) in enumerate(groups):
        for slot in range(start, start + count):
            if slot != low_z:
                remote(own, ubuf.at[y, slot], u_send.at[0], u_recv.at[slot], me, t).wait_recv()
        span = pl.ds(start, count)
        for d in range(1, ny):
            go(remote(
                ubuf.at[y, span], ubuf.at[y, span], v_send.at[g, d], v_recv.at[g, y], fs_at(0, d), t
            ))
        for slot in range(start, start + count):
            if slot != low_z:
                squares += ubuf[y, slot] * ubuf[y, slot]
    sums[y, t] = jnp.sum(squares, axis=0, keepdims=True)
    for d in range(tp - 1, -1, -1):
        for e in range(ny - 1, -1, -1):
            if d > 0 or e > 0:
                go(remote(
                    sums.at[y, t], sums.at[y, t], q_send.at[e, d], q_recv.at[y, t], fs_at(0, e), (t + d) % tp
                ))

    def place(k, start, count):
        for slot in range(start, start + count):
            at = pl.multiple_of((z + slot - low_z + nz) % nz * (ny * rr) + k * rr, rr)
            ufull[at // rr] = ubuf[k, slot]

    for g, (start, count) in enumerate(groups):
        place(y, start, count)
    for g, (start, count) in enumerate(groups):
        span = pl.ds(start, count)
        for d in range(1, ny):
            k = (y + d) % ny
            remote(ubuf.at[k, span], ubuf.at[k, span], v_send.at[g, 0], v_recv.at[g, k], me, t).wait_recv()
            place(k, start, count)

    full = jnp.concatenate([ufull[i] for i in range(nz * ny)], axis=0)
    high, low_bits = split2(full)
    product = jnp.dot(bv[...], high, preferred_element_type=f32)
    product += jnp.dot(bv[...], low_bits, preferred_element_type=f32)
    product_ref[...] = product

    for d in range(tp):
        for e in range(ny):
            if d > 0 or e > 0:
                k, i = (y + e) % ny, (t + d) % tp
                remote(sums.at[k, i], sums.at[k, i], q_send.at[0, 0], q_recv.at[k, i], me, t).wait_recv()
    head = sums[0, t]
    for k in range(1, ny):
        head += sums[k, t]
    whole = jnp.zeros_like(head)
    for i in range(tp):
        for k in range(ny):
            whole += sums[k, i]
    head = jnp.sum(head, axis=1, keepdims=True) / (rank * DQK)
    whole = jnp.sum(whole, axis=1, keepdims=True) / (rank * cols * tp)
    factor_ref[...] = jnp.broadcast_to(1.0 / jnp.sqrt(head + whole), factor_ref.shape)

    for copy in sent:
        copy.wait_send()


def finish(
    product_ref, factor_ref, low_ref, first_ref, second_ref, master_ref,
    step_ref, first_out, second_out, copy_ref,
):
    first_out[...], second_out[...] = moments(first_ref[...], second_ref[...], low_ref[...])
    step = product_ref[...] * factor_ref[:1]
    step_ref[...] = step
    copy_ref[...] = (master_ref[...] + step).astype(jnp.bfloat16)


def body(n, tp, inputs, query_cot, query_basis, query_master, query_first, query_second):
    ny = NY
    nz = n // ny
    tokens, width = inputs.shape
    rows, rank = query_basis.shape
    rr, cols = query_first.shape
    tall = rank // tp // ny
    f32, bf16 = jnp.float32, jnp.bfloat16
    dma = pltpu.SemaphoreType.DMA
    vmem = pl.BlockSpec(memory_space=pltpu.VMEM)
    hbm = pl.BlockSpec(memory_space=pl.ANY)
    product, factor, low = pl.pallas_call(
        functools.partial(kernel, nz, ny, tp),
        out_shape=(
            jax.ShapeDtypeStruct((rows, cols), f32),
            jax.ShapeDtypeStruct((8, cols), f32),
            jax.ShapeDtypeStruct((rr, cols), f32),
        ),
        in_specs=[hbm] * 5,
        out_specs=(vmem,) * 3,
        scratch_shapes=[
            pltpu.VMEM((tokens, width), bf16),
            pltpu.VMEM((tp, tokens, cols), bf16),
            pltpu.VMEM((rows, rank), bf16),
            pltpu.VMEM((rr, cols), f32),
            pltpu.VMEM((rr, cols), f32),
            pltpu.VMEM((ny, nz, 8, LANES), bf16),
            pltpu.VMEM((n * rows, LANES), bf16),
            pltpu.VMEM((ny, tp, tall, cols), f32),
            pltpu.VMEM((ny, tp, tall, cols), f32),
            pltpu.VMEM((nz, rr, cols), f32),
            pltpu.VMEM((nz, rr, cols), f32),
            pltpu.VMEM((ny, nz, rr, cols), f32),
            pltpu.VMEM((n, rr, cols), f32),
            pltpu.VMEM((ny, tp, 1, cols), f32),
            dma((5,)),
            dma((2 * REACH,)), dma((nz,)),
            dma((2,)), dma((2,)),
            dma((3, ny)), dma((3, ny)),
            dma((tp,)), dma((tp,)),
            dma((tp, ny)), dma((ny, tp)),
            dma((nz,)), dma((nz,)),
            dma((nz,)), dma((nz,)),
            dma((5, ny)), dma((5, ny)),
            dma((ny, tp)), dma((ny, tp)),
        ],
        compiler_params=pltpu.CompilerParams(collective_id=0, has_side_effects=True),
    )(inputs, query_cot, query_basis, query_first, query_second)
    return pl.pallas_call(
        finish,
        out_shape=(
            jax.ShapeDtypeStruct((rows, cols), f32),
            jax.ShapeDtypeStruct((rr, cols), f32),
            jax.ShapeDtypeStruct((rr, cols), f32),
            jax.ShapeDtypeStruct((rows, cols), bf16),
        ),
        in_specs=[vmem] * 6,
        out_specs=(vmem,) * 4,
    )(product, factor, low, query_first, query_second, query_master)


def solution(mesh):
    placed = (
        P("fs", None),
        P("fs", "tp"),
        P("fs", None),
        P("fs", "tp"),
        P("fs", "tp"),
        P("fs", "tp"),
    )
    return jax.shard_map(
        functools.partial(body, mesh.shape["fs"], mesh.shape["tp"]),
        mesh=mesh,
        in_specs=placed,
        out_specs=(P("fs", "tp"),) * 4,
        check_vma=False,
    )
```
